32 devices in a mesh: fs: 8 (over z, y), tp: 4 (over x, core).
Axes of the slice: x: 2, y: 2, z: 4, core: 2. Of those that a mesh axis runs over, the one named last changes fastest.
Arguments:
- stream_in: bfloat16 [2048, 2112], P('fs'), may hold values from -6 to 6
- norm_gains: float32 [6, 2112], replicated, may hold values from 0.1 to 1.9
- gate_proj: bfloat16 [2112, 3072], P('fs', 'tp'), may hold values from -0.125 to 0.125
- up_proj: bfloat16 [2112, 3072], P('fs', 'tp'), may hold values from -0.125 to 0.125
- down_proj: bfloat16 [2112, 3072], P('fs', 'tp'), may hold values from -0.109375 to 0.109375
- outer_gate: bfloat16 [2112, 1056], P('fs', 'tp'), may hold values from -0.125 to 0.125
- inner_gate: bfloat16 [2112, 1056], P('fs', 'tp'), may hold values from -0.125 to 0.125
- value_proj: bfloat16 [2112, 1056], P('fs', 'tp'), may hold values from -0.125 to 0.125
- mixer_out: bfloat16 [2112, 1056], P('fs', 'tp'), may hold values from -0.1875 to 0.1875
- conv_taps: bfloat16 [3, 1056], replicated, may hold values from -3 to 3
Outputs:
- stream_out: bfloat16 [2048, 2112], P('fs')
The draws below stay inside these ranges and needn't reach their ends.
All inputs are finite; a program needn't handle non-finite values.
Results may differ from the reference program's by a relative error of at most 0.02.
Values may be sent and summed in bfloat16 or wider, within the bound.
A program may use at most 64 MiB of HBM per device.

```python
import jax
import jax.numpy as jnp
from jax import lax

D = 2112
FF = 3072
CW = 1056
CONV_K = 3
ROWS = 256
TOKENS = 2048
N_FS = 8
N_TP = 4


def shard_levels(key, dims, split, low, high):
    factor_of, own = 1.0, jax.random.fold_in(key, 6)
    for position, parts in split:
        steps = jnp.exp(jax.random.uniform(jax.random.fold_in(own, position), (parts,), jnp.float32, low / len(split), high / len(split)))
        factor_of = factor_of * jnp.repeat(steps, dims[position] // parts).reshape([-1 if axis == position else 1 for axis in range(len(dims))])
    return factor_of


def bell_draw(own_key, dims, width, most, split=(), held_as=jnp.bfloat16):
    values = jax.random.normal(own_key, dims, jnp.float32) * width
    if len(split) > 0:
        values = shard_levels(own_key, dims, split, -0.22, 0.18) * values
    return jnp.clip(values, min=-most, max=most).astype(held_as)


def setup_inputs(seed: int = 0) -> dict:
    key_of = jax.random.split(jax.random.key(seed), 11)
    stream_in = bell_draw(key_of[0], (TOKENS, D), 1.0, 6.0, ((0, 8),))
    norm_gains = jnp.clip(1.0 + 0.18 * jax.random.normal(key_of[1], (6, D), jnp.float32), 0.1, 1.9)
    gate_proj = bell_draw(key_of[2], (D, FF), D ** -0.5, 0.125, ((0, 8), (1, 4)))
    up_proj = bell_draw(key_of[3], (D, FF), D ** -0.5, 0.125, ((0, 8), (1, 4)))
    down_proj = bell_draw(key_of[4], (D, FF), FF ** -0.5, 0.109375, ((0, 8), (1, 4)))
    outer_gate = bell_draw(key_of[5], (D, CW), D ** -0.5, 0.125, ((0, 8), (1, 4)))
    inner_gate = bell_draw(key_of[6], (D, CW), D ** -0.5, 0.125, ((0, 8), (1, 4)))
    value_proj = bell_draw(key_of[7], (D, CW), D ** -0.5, 0.125, ((0, 8), (1, 4)))
    mixer_out = bell_draw(key_of[8], (D, CW), CW ** -0.5, 0.1875, ((0, 8), (1, 4)))
    conv_taps = bell_draw(key_of[9], (CONV_K, CW), 0.577, 3.0)
    return dict(stream_in=stream_in, norm_gains=norm_gains, gate_proj=gate_proj, up_proj=up_proj, down_proj=down_proj, outer_gate=outer_gate, inner_gate=inner_gate, value_proj=value_proj, mixer_out=mixer_out, conv_taps=conv_taps)


EPSILON = 1e-06

def scaled(values, gain):
    return values * lax.rsqrt(lax.optimization_barrier(jnp.mean(values * values, axis=-1, keepdims=True)) + EPSILON) * gain

def block_sum(inner, weight):
    span_width = inner.shape[1] // N_TP
    total = jnp.zeros((inner.shape[0], weight.shape[0]), jnp.float32)
    for shard_index in range(N_TP):
        left = inner[:, shard_index * span_width:(shard_index + 1) * span_width]
        right = weight[:, shard_index * span_width:(shard_index + 1) * span_width]
        part = lax.dot_general(left, right, (((1,), (1,)), ((), ())), preferred_element_type=jnp.float32)
        total = total + lax.optimization_barrier(part.astype(jnp.bfloat16)).astype(jnp.float32)
    return total

def half_step(stream, norm_gains, first, gate_proj, up_proj, down_proj):
    normed = scaled(stream.astype(jnp.float32), norm_gains[first]).astype(jnp.bfloat16)
    gate = jnp.dot(normed, gate_proj, preferred_element_type=jnp.float32)
    upward = jnp.dot(normed, up_proj, preferred_element_type=jnp.float32)
    hidden = (jax.nn.silu(gate) * upward).astype(jnp.bfloat16)
    summed = block_sum(hidden, down_proj)
    result = stream.astype(jnp.float32) + 0.5 * scaled(summed, norm_gains[first + 1])
    return result.astype(jnp.bfloat16)

def reference(stream_in, norm_gains, gate_proj, up_proj, down_proj, outer_gate, inner_gate, value_proj, mixer_out, conv_taps):
    after_ffn = half_step(stream_in, norm_gains, 0, gate_proj, up_proj, down_proj)
    normed = scaled(after_ffn.astype(jnp.float32), norm_gains[2]).astype(jnp.bfloat16)
    outer = jnp.dot(normed, outer_gate, preferred_element_type=jnp.float32).astype(jnp.bfloat16)
    inner = jnp.dot(normed, inner_gate, preferred_element_type=jnp.float32).astype(jnp.bfloat16)
    value = jnp.dot(normed, value_proj, preferred_element_type=jnp.float32).astype(jnp.bfloat16)
    gated = (inner.astype(jnp.float32) * value.astype(jnp.float32)).reshape(N_FS, ROWS, CW)
    padded = jnp.pad(gated, ((0, 0), (CONV_K - 1, 0), (0, 0)))
    taps = conv_taps.astype(jnp.float32)
    conv = jnp.zeros_like(gated)
    for offset in range(CONV_K):
        conv = conv + taps[offset] * padded[:, offset:offset + ROWS]
    mixed = (outer.astype(jnp.float32) * conv.reshape(N_FS * ROWS, CW)).astype(jnp.bfloat16)
    summed = block_sum(mixed, mixer_out)
    after_mixer = (after_ffn.astype(jnp.float32) + scaled(summed, norm_gains[3])).astype(jnp.bfloat16)
    return half_step(after_mixer, norm_gains, 4, gate_proj, up_proj, down_proj)
```

```python
import functools

import jax
import jax.numpy as jnp
from jax import lax
from jax.experimental import pallas as pl
from jax.experimental.pallas import tpu as pltpu
from jax.sharding import PartitionSpec as P

MESH = pl.DeviceIdType.MESH
EPSILON = 1e-06
CONV_K = 3
F32, BF16 = jnp.float32, jnp.bfloat16
NT = (((1,), (1,)), ((), ()))


def kernel(cfg, *refs):
    Z, Y, X, shard, width, hc, nff, main, rem = cfg
    own_refs = refs[: nff + 2]
    stream_ref, gains_ref, taps_ref, out_ref = refs[nff + 2 : nff + 6]
    (ff, g3, g4, normed, acc, hidden, csend, crecv, xsend, xrecv, res,
     lsem, zsend, recv, asend, arecv, csem, xssem, xrsem, rsem) = refs[nff + 6 :]
    rows, Dp = stream_ref.shape
    half = rows // 2
    K3, K4 = nff, nff + 1
    f, t = lax.axis_index("fs"), lax.axis_index("tp")
    z, y = f // Y, f % Y
    c, x = t % 2, t // 2
    core_peer = (f, x * 2 + 1 - c)
    x_peers = [(f, ((x + j) % X) * 2 + c) for j in range(1, X)]

    def dev_z(zz):
        return (zz * Y + y, t)

    dev_y = (z * Y + (Y - 1 - y), t)

    barrier = pltpu.get_barrier_semaphore()

    def greet(d):
        pl.semaphore_signal(barrier, inc=1, device_id=d, device_id_type=MESH)

    always = [core_peer] + x_peers + ([dev_y] if Y == 2 else [])
    for d in always:
        greet(d)
    if Z > 1:
        @pl.when(z > 0)
        def _():
            greet(dev_z(z - 1))

        @pl.when(z < Z - 1)
        def _():
            greet(dev_z(z + 1))

    def slot(k, first, count):
        at = pl.ds(pl.multiple_of(first * shard, 16), count * shard)
        if k < nff:
            return ff.at[k, at]
        return (g3 if k == K3 else g4).at[at]

    local = [
        pltpu.make_async_copy(own_refs[k], slot(k, f, 1), lsem.at[k]) for k in range(nff + 2)
    ]
    for copy in local:
        copy.start()

    peers = len(always)
    if Z > 1:
        peers = peers + (z > 0).astype(jnp.int32) + (z < Z - 1).astype(jnp.int32)
    pl.semaphore_wait(barrier, peers)

    def remote(k, s, way, d):
        ref = slot(k, s, 1)
        return pltpu.make_async_remote_copy(
            src_ref=ref, dst_ref=ref, send_sem=zsend.at[k, way, s], recv_sem=recv.at[k, s],
            device_id=d, device_id_type=MESH,
        )

    def remote_a(s, way, d):
        ref = slot(K4, s * Y, Y)
        return pltpu.make_async_remote_copy(
            src_ref=ref, dst_ref=ref, send_sem=asend.at[way, s], recv_sem=arecv.at[s],
            device_id=d, device_id_type=MESH,
        )

    def right(k, s, act):
        @pl.when(z < Z - 1)
        def _():
            act(remote(k, s * Y + y, 0, dev_z(z + 1)))

    def left(k, s, act):
        @pl.when(z > 0)
        def _():
            act(remote(k, s * Y + y, 1, dev_z(z - 1)))

    def across(k, s, act):
        if Y == 2:
            act(remote(k, s * Y + y, 2, dev_y))

    def go(copy):
        copy.start()

    def own(k):
        right(k, z, go)
        left(k, z, go)
        across(k, z, go)

    def zsteps(k):
        def step(i, carry):
            @pl.when(z - 1 - i >= 0)
            def _():
                s = z - 1 - i
                remote(k, s * Y + y, 0, dev_z(z - 1)).wait_recv()
                right(k, s, go)
                across(k, s, go)

            @pl.when(z + 1 + i < Z)
            def _():
                s = z + 1 + i
                remote(k, s * Y + y, 0, dev_z(z + 1)).wait_recv()
                left(k, s, go)
                across(k, s, go)

            return carry

        lax.fori_loop(0, Z - 1, step, 0)

    def wait_across(k):
        if Y == 2:
            def step(s, carry):
                remote(k, s * Y + 1 - y, 2, dev_y).wait_recv()
                return carry

            lax.fori_loop(0, Z, step, 0)

    def right_a(s, act):
        @pl.when(z < Z - 1)
        def _():
            act(remote_a(s, 0, dev_z(z + 1)))

    def left_a(s, act):
        @pl.when(z > 0)
        def _():
            act(remote_a(s, 1, dev_z(z - 1)))

    def start_a():
        if Y == 2:
            remote(K4, z * Y + 1 - y, 2, dev_y).wait_recv()
        right_a(z, go)
        left_a(z, go)

    def steps_a(forward):
        def step(i, carry):
            @pl.when((z - 1 - i >= 0) & ((z < Z - 1) if forward else (z == Z - 1)))
            def _():
                s = z - 1 - i
                remote_a(s, 0, dev_z(z - 1)).wait_recv()
                if forward:
                    right_a(s, go)

            @pl.when((z + 1 + i < Z) & ((z > 0) if forward else (z == 0)))
            def _():
                s = z + 1 + i
                remote_a(s, 0, dev_z(z + 1)).wait_recv()
                if forward:
                    left_a(s, go)

            return carry

        lax.fori_loop(0, Z - 1, step, 0)

    def scaled(values, row):
        mean = jnp.sum(values * values, axis=-1, keepdims=True) * (1.0 / width)
        return values * lax.rsqrt(mean + EPSILON) * gains_ref[row : row + 1, :]

    def norm_to(source, row):
        def block(i, carry):
            at = pl.ds(pl.multiple_of(i * 32, 32), 32)
            normed[at] = scaled(source[at].astype(F32), row).astype(BF16)
            return carry

        lax.fori_loop(0, rows // 32, block, 0)

    def ffn_chunk(k, first):
        weights = ff.at[k]

        def block(i, carry):
            at = pl.ds(pl.multiple_of(i * half, 16), half)
            n = normed[at]
            gate = jnp.dot(n, weights[:, 0:hc], preferred_element_type=F32)
            up = jnp.dot(n, weights[:, hc : 2 * hc], preferred_element_type=F32)
            h = (gate / (1.0 + jnp.exp(-gate)) * up).astype(BF16)
            part = lax.dot_general(h, weights[:, 2 * hc :], NT, preferred_element_type=F32)
            acc[at] = part if first else acc[at] + part
            return carry

        lax.fori_loop(0, 2, block, 0)

    mine = pl.ds(pl.multiple_of(c * half, 16), half)
    other = pl.ds(pl.multiple_of((1 - c) * half, 16), half)

    def reduce(r, source, row, factor):
        csend[r] = acc[other].astype(BF16)
        first = pltpu.make_async_remote_copy(
            src_ref=csend.at[r], dst_ref=crecv.at[r], send_sem=csem.at[0, r],
            recv_sem=csem.at[1, r], device_id=core_peer, device_id_type=MESH,
        )
        first.start()
        first.wait()
        xsend[r] = (acc[mine].astype(BF16).astype(F32) + crecv[r].astype(F32)).astype(BF16)
        sends = []
        for j, peer in enumerate(x_peers):
            copy = pltpu.make_async_remote_copy(
                src_ref=xsend.at[r], dst_ref=xrecv.at[r, j], send_sem=xssem.at[r, j],
                recv_sem=xrsem.at[r, j], device_id=peer, device_id_type=MESH,
            )
            copy.start()
            sends.append(copy)
        for copy in sends:
            copy.wait()

        def block(i, carry):
            at = pl.ds(pl.multiple_of(i * 32, 16), 32)
            full = pl.ds(pl.multiple_of(c * half + i * 32, 16), 32)
            total = xsend[r, at].astype(F32)
            for j in range(X - 1):
                total = total + xrecv[r, j, at].astype(F32)
            res[r, full] = (
                source[full].astype(F32) + factor * scaled(total, row)
            ).astype(BF16)
            return carry

        lax.fori_loop(0, half // 32, block, 0)
        last = pltpu.make_async_remote_copy(
            src_ref=res.at[r, mine], dst_ref=res.at[r, mine], send_sem=rsem.at[0, r],
            recv_sem=rsem.at[1, r], device_id=core_peer, device_id_type=MESH,
        )
        last.start()
        last.wait_send()
        pltpu.make_async_remote_copy(
            src_ref=res.at[r, other], dst_ref=res.at[r, other], send_sem=rsem.at[0, r],
            recv_sem=rsem.at[1, r], device_id=core_peer, device_id_type=MESH,
        ).wait_recv()

    def mixer():
        edge = main + 128
        outer_inner = jnp.dot(normed[...], g3[...], preferred_element_type=F32)
        outer_inner = outer_inner.astype(BF16).astype(F32)
        value_rest = jnp.dot(normed[...], g4[:, 0:edge], preferred_element_type=F32)
        value_rest = value_rest.astype(BF16).astype(F32)
        rest = value_rest[:, main:]
        if rem:
            lane = lax.broadcasted_iota(jnp.int32, rest.shape, 1)
            keep = (lane >= 3 * rem) & (lane < 4 * rem)
            rests = [
                jnp.where(keep, pltpu.roll(rest, (3 - j) * rem, 1), 0.0) for j in range(3)
            ]
        else:
            rests = [jnp.zeros_like(rest)] * 3
        outer = jnp.concatenate([rests[0], outer_inner[:, 0:main]], axis=1)
        inner = jnp.concatenate([rests[1], outer_inner[:, main:]], axis=1)
        value = jnp.concatenate([rests[2], value_rest[:, 0:main]], axis=1)
        gated = inner * value
        token = lax.broadcasted_iota(jnp.int32, gated.shape, 0)
        conv = jnp.zeros_like(gated)
        for j in range(CONV_K):
            back = CONV_K - 1 - j
            moved = gated
            if back:
                moved = jnp.where(token >= back, pltpu.roll(gated, back, 0), 0.0)
            conv = conv + taps_ref[j : j + 1, :] * moved
        hidden[...] = (outer * conv).astype(BF16)

        def block(i, carry):
            at = pl.ds(pl.multiple_of(i * half, 16), half)
            acc[at] = lax.dot_general(
                hidden[at], g4[:, main:], NT, preferred_element_type=F32
            )
            return carry

        lax.fori_loop(0, 2, block, 0)

    for k, copy in enumerate(local):
        copy.wait()
        if k < 2:
            own(k)
    norm_to(stream_ref, 0)
    for k in range(nff):
        zsteps(k)
        if k + 2 <= K3:
            own(k + 2)
        if k + 2 == K3:
            across(K4, z, go)
        if k > 0:
            wait_across(k - 1)
            ffn_chunk(k - 1, k == 1)
    zsteps(K3)
    start_a()
    steps_a(True)
    wait_across(nff - 1)
    ffn_chunk(nff - 1, nff == 1)
    reduce(0, stream_ref, 1, 0.5)
    norm_to(res.at[0], 2)
    wait_across(K3)
    steps_a(False)
    mixer()
    reduce(1, res.at[0], 3, 1.0)
    norm_to(res.at[1], 4)
    acc[...] = jnp.zeros_like(acc)

    def again(k, carry):
        ffn_chunk(k, False)
        return carry

    lax.fori_loop(0, nff, again, 0)
    reduce(2, res.at[1], 5, 0.5)
    out_ref[...] = res[2]

    def done(copy):
        copy.wait_send()

    for k in range(nff + 1):
        def drain(s, carry):
            @pl.when(s <= z)
            def _():
                right(k, s, done)

            @pl.when(s >= z)
            def _():
                left(k, s, done)

            across(k, s, done)
            return carry

        lax.fori_loop(0, Z, drain, 0)
    across(K4, z, done)

    def drain_a(s, carry):
        @pl.when(s <= z)
        def _():
            right_a(s, done)

        @pl.when(s >= z)
        def _():
            left_a(s, done)

        return carry

    lax.fori_loop(0, Z, drain_a, 0)


def y_count(mesh):
    try:
        found = len({d.coords[1] for d in mesh.devices.reshape(-1)})
    except AttributeError:
        found = 1
    return found if found == 2 and mesh.shape["fs"] % 2 == 0 else 1


def solution(mesh):
    n_fs, n_tp = mesh.shape["fs"], mesh.shape["tp"]
    Y = y_count(mesh)
    Z, X = n_fs // Y, n_tp // 2

    def local(stream_in, norm_gains, gate, up, down, outer_w, inner_w, value_w, mixer_w, conv_taps):
        rows, width = stream_in.shape
        part, hid = gate.shape
        channels = outer_w.shape[1]
        shard = -(-part // 16) * 16
        Dp = n_fs * shard
        nff = 3 if hid % 384 == 0 else 1
        hc = hid // nff
        main = channels // 128 * 128
        rem = channels - main

        def widen(v):
            lead = v.shape[0]
            v = v.reshape(lead, n_fs, part)
            return jnp.pad(v, ((0, 0), (0, 0), (0, shard - part))).reshape(lead, Dp)

        def pack(parts):
            w = jnp.concatenate(parts, axis=1)
            return jnp.pad(w, ((0, shard - part), (0, 0)))

        owns = [
            pack([w[:, k * hc : (k + 1) * hc] for w in (gate, up, down)]) for k in range(nff)
        ]
        owns.append(pack([outer_w[:, :main], inner_w[:, :main]]))
        rest = [w[:, main:] for w in (outer_w, inner_w, value_w, mixer_w)]
        rest.append(jnp.zeros((part, 128 - 4 * rem), BF16))
        owns.append(pack([value_w[:, :main]] + rest + [mixer_w[:, :main]]))
        taps = lax.dynamic_slice_in_dim(
            conv_taps, lax.axis_index("tp") * channels, channels, 1
        ).astype(F32)
        taps = jnp.concatenate(
            [jnp.pad(taps[:, main:], ((0, 0), (3 * rem, 128 - 4 * rem))), taps[:, :main]], axis=1
        )
        half = rows // 2
        dma, vmem = pltpu.SemaphoreType.DMA, pltpu.VMEM
        out = pl.pallas_call(
            functools.partial(kernel, (Z, Y, X, shard, width, hc, nff, main, rem)),
            out_shape=jax.ShapeDtypeStruct((rows, Dp), BF16),
            in_specs=[pl.BlockSpec(memory_space=pl.ANY)] * (nff + 2)
            + [pl.BlockSpec(memory_space=pltpu.VMEM)] * 3,
            out_specs=pl.BlockSpec(memory_space=pltpu.VMEM),
            scratch_shapes=[
                vmem((nff, Dp, 3 * hc), BF16),
                vmem((Dp, 2 * main), BF16),
                vmem((Dp, 2 * main + 128), BF16),
                vmem((rows, Dp), BF16),
                vmem((rows, Dp), F32),
                vmem((rows, main + 128), BF16),
                vmem((3, half, Dp), BF16),
                vmem((3, half, Dp), BF16),
                vmem((3, half, Dp), BF16),
                vmem((3, X - 1, half, Dp), BF16),
                vmem((3, rows, Dp), BF16),
                dma((nff + 2,)),
                dma((nff + 2, 3, n_fs)),
                dma((nff + 2, n_fs)),
                dma((2, Z)),
                dma((Z,)),
                dma((2, 3)),
                dma((3, X - 1)),
                dma((3, X - 1)),
                dma((2, 3)),
            ],
            compiler_params=pltpu.CompilerParams(
                collective_id=0, has_side_effects=True, vmem_limit_bytes=60 * 1024 * 1024
            ),
        )(*owns, widen(stream_in), widen(norm_gains), taps)
        return out.reshape(rows, n_fs, shard)[:, :, :part].reshape(rows, width)

    return jax.shard_map(
        local,
        mesh=mesh,
        in_specs=(P("fs", None), P()) + (P("fs", "tp"),) * 7 + (P(),),
        out_specs=P("fs", None),
        check_vma=False,
    )
```

```python
import functools

import jax
import jax.numpy as jnp
from jax import lax
from jax.experimental import pallas as pl
from jax.experimental.pallas import tpu as pltpu
from jax.sharding import PartitionSpec as P

MESH = pl.DeviceIdType.MESH
EPSILON = 1e-06
CONV_K = 3
F32, BF16 = jnp.float32, jnp.bfloat16
NT = (((1,), (1,)), ((), ()))


def kernel(cfg, *refs):
    Z, Y, X, shard, sent, width, hc, nff, main, rem = cfg
    own_refs = refs[:8]
    stream_ref, gains_ref, taps_ref, out_ref = refs[8:12]
    (ff, g3, g4, normed, acc, hidden, csend, crecv, xsend, xrecv, res,
     lsem, zsend, recv, asend, arecv, csem, xssem, xrsem, rsem) = refs[12:]
    rows, Dp = stream_ref.shape
    half, quarter = rows // 2, rows // 4
    K3, K4 = nff, nff + 1
    f, t = lax.axis_index("fs"), lax.axis_index("tp")
    z, y = f // Y, f % Y
    c, x = t % 2, t // 2
    core_peer = (f, x * 2 + 1 - c)
    x_peers = [(f, ((x + j) % X) * 2 + c) for j in range(1, X)]

    def dev_z(zz):
        return (zz * Y + y, t)

    dev_y = (z * Y + (Y - 1 - y), t)

    for s in range(Z * Y):
        tail = pl.ds(s * shard + shard - 16, 16)
        for k in range(nff):
            ff[k, tail] = jnp.zeros((16, 3 * hc), BF16)
        g3[tail] = jnp.zeros((16, 2 * main), BF16)
        g4[tail] = jnp.zeros((16, 2 * main + 128), BF16)

    barrier = pltpu.get_barrier_semaphore()

    def greet(d):
        pl.semaphore_signal(barrier, inc=1, device_id=d, device_id_type=MESH)

    always = [core_peer] + x_peers + ([dev_y] if Y == 2 else [])
    for d in always:
        greet(d)
    if Z > 1:
        @pl.when(z > 0)
        def _():
            greet(dev_z(z - 1))

        @pl.when(z < Z - 1)
        def _():
            greet(dev_z(z + 1))

    def slot(k, first, count):
        at = pl.ds(pl.multiple_of(first * shard, 16), (count - 1) * shard + sent)
        if k < nff:
            return ff.at[k, at]
        return (g3 if k == K3 else g4).at[at]

    here = pl.ds(pl.multiple_of(f * shard, 16), sent)
    moves = []
    for k in range(nff):
        for j in range(3):
            moves.append((k, own_refs[j].at[:, pl.ds(k * hc, hc)],
                          ff.at[k, here, pl.ds(j * hc, hc)]))
    ow, iw, vw, mw, rw = own_refs[3:]
    lead = pl.ds(0, main)
    moves.append((K3, ow.at[:, lead], g3.at[here, lead]))
    moves.append((K3, iw.at[:, lead], g3.at[here, pl.ds(main, main)]))
    moves.append((K4, vw.at[:, lead], g4.at[here, lead]))
    moves.append((K4, rw, g4.at[here, pl.ds(main, 128)]))
    moves.append((K4, mw.at[:, lead], g4.at[here, pl.ds(main + 128, main)]))
    local = [
        (k, pltpu.make_async_copy(src, dst, lsem.at[n])) for n, (k, src, dst) in enumerate(moves)
    ]
    for _, copy in local:
        copy.start()

    peers = len(always)
    if Z > 1:
        peers = peers + (z > 0).astype(jnp.int32) + (z < Z - 1).astype(jnp.int32)
    pl.semaphore_wait(barrier, peers)

    def remote(k, s, way, d):
        ref = slot(k, s, 1)
        return pltpu.make_async_remote_copy(
            src_ref=ref, dst_ref=ref, send_sem=zsend.at[k, way, s], recv_sem=recv.at[k, s],
            device_id=d, device_id_type=MESH,
        )

    def remote_a(s, way, d):
        ref = slot(K4, s * Y, Y)
        return pltpu.make_async_remote_copy(
            src_ref=ref, dst_ref=ref, send_sem=asend.at[way, s], recv_sem=arecv.at[s],
            device_id=d, device_id_type=MESH,
        )

    def right(k, s, act):
        @pl.when(z < Z - 1)
        def _():
            act(remote(k, s * Y + y, 0, dev_z(z + 1)))

    def left(k, s, act):
        @pl.when(z > 0)
        def _():
            act(remote(k, s * Y + y, 1, dev_z(z - 1)))

    def across(k, s, act):
        if Y == 2:
            act(remote(k, s * Y + y, 2, dev_y))

    def go(copy):
        copy.start()

    def own(k):
        right(k, z, go)
        left(k, z, go)
        across(k, z, go)

    def zsteps(k):
        def step(i, carry):
            @pl.when(z - 1 - i >= 0)
            def _():
                s = z - 1 - i
                remote(k, s * Y + y, 0, dev_z(z - 1)).wait_recv()
                right(k, s, go)
                across(k, s, go)

            @pl.when(z + 1 + i < Z)
            def _():
                s = z + 1 + i
                remote(k, s * Y + y, 0, dev_z(z + 1)).wait_recv()
                left(k, s, go)
                across(k, s, go)

            return carry

        lax.fori_loop(0, Z - 1, step, 0)

    def wait_across(k):
        if Y == 2:
            def step(s, carry):
                remote(k, s * Y + 1 - y, 2, dev_y).wait_recv()
                return carry

            lax.fori_loop(0, Z, step, 0)

    def right_a(s, act):
        @pl.when(z < Z - 1)
        def _():
            act(remote_a(s, 0, dev_z(z + 1)))

    def left_a(s, act):
        @pl.when(z > 0)
        def _():
            act(remote_a(s, 1, dev_z(z - 1)))

    def start_a():
        if Y == 2:
            remote(K4, z * Y + 1 - y, 2, dev_y).wait_recv()
        right_a(z, go)
        left_a(z, go)

    def steps_a(forward):
        def step(i, carry):
            @pl.when((z - 1 - i >= 0) & ((z < Z - 1) if forward else (z == Z - 1)))
            def _():
                s = z - 1 - i
                remote_a(s, 0, dev_z(z - 1)).wait_recv()
                if forward:
                    right_a(s, go)

            @pl.when((z + 1 + i < Z) & ((z > 0) if forward else (z == 0)))
            def _():
                s = z + 1 + i
                remote_a(s, 0, dev_z(z + 1)).wait_recv()
                if forward:
                    left_a(s, go)

            return carry

        lax.fori_loop(0, Z - 1, step, 0)

    def scaled(values, row):
        mean = jnp.sum(values * values, axis=-1, keepdims=True) * (1.0 / width)
        return values * lax.rsqrt(mean + EPSILON) * gains_ref[row : row + 1, :]

    def norm_to(source, row):
        def block(i, carry):
            at = pl.ds(pl.multiple_of(i * 32, 32), 32)
            per_half, per_quarter = half // 32, quarter // 32
            h, b = i // per_half, (i % per_half) // per_quarter
            to = pl.ds(pl.multiple_of(h * quarter + (i % per_quarter) * 32, 32), 32)
            normed[b, to] = scaled(source[at].astype(F32), row).astype(BF16)
            return carry

        lax.fori_loop(0, rows // 32, block, 0)

    def ffn_block(k, b, first):
        weights = ff.at[k]
        n = normed[b]
        gate = jnp.dot(n, weights[:, 0:hc], preferred_element_type=F32)
        up = jnp.dot(n, weights[:, hc : 2 * hc], preferred_element_type=F32)
        h = (gate / (1.0 + jnp.exp(-gate)) * up).astype(BF16)
        part = lax.dot_general(h, weights[:, 2 * hc :], NT, preferred_element_type=F32)
        acc[b] = part if first else acc[b] + part

    def ffn_chunk(k, first):
        def block(b, carry):
            ffn_block(k, b, first)
            return carry

        lax.fori_loop(0, 2, block, 0)

    mine = pl.ds(pl.multiple_of(c * quarter, 16), quarter)
    other = pl.ds(pl.multiple_of((1 - c) * quarter, 16), quarter)

    def core_copy(r, b):
        return pltpu.make_async_remote_copy(
            src_ref=csend.at[r, b], dst_ref=crecv.at[r, b], send_sem=csem.at[0, r, b],
            recv_sem=csem.at[1, r, b], device_id=core_peer, device_id_type=MESH,
        )

    def x_copy(r, b, j):
        return pltpu.make_async_remote_copy(
            src_ref=xsend.at[r, b], dst_ref=xrecv.at[r, b, j], send_sem=xssem.at[r, b, j],
            recv_sem=xrsem.at[r, b, j], device_id=x_peers[j], device_id_type=MESH,
        )

    def res_copy(r, b, core):
        at = pl.ds(pl.multiple_of(core * half + b * quarter, 16), quarter)
        return pltpu.make_async_remote_copy(
            src_ref=res.at[r, at], dst_ref=res.at[r, at], send_sem=rsem.at[0, r, b],
            recv_sem=rsem.at[1, r, b], device_id=core_peer, device_id_type=MESH,
        )

    def reduce(r, compute, source, row, factor):
        def send(b, carry):
            compute(b)
            csend[r, b] = acc[b, other].astype(BF16)
            core_copy(r, b).start()
            core_copy(r, b).wait()
            xsend[r, b] = (
                acc[b, mine].astype(BF16).astype(F32) + crecv[r, b].astype(F32)
            ).astype(BF16)
            for j in range(X - 1):
                x_copy(r, b, j).start()
            return carry

        def receive(b, carry):
            for j in range(X - 1):
                x_copy(r, b, j).wait()

            def block(i, inner_carry):
                at = pl.ds(pl.multiple_of(i * 32, 16), 32)
                full = pl.ds(pl.multiple_of(c * half + b * quarter + i * 32, 16), 32)
                total = xsend[r, b, at].astype(F32)
                for j in range(X - 1):
                    total = total + xrecv[r, b, j, at].astype(F32)
                res[r, full] = (
                    source[full].astype(F32) + factor * scaled(total, row)
                ).astype(BF16)
                return inner_carry

            lax.fori_loop(0, quarter // 32, block, 0)
            res_copy(r, b, c).start()
            return carry

        def finish(b, carry):
            res_copy(r, b, c).wait_send()
            res_copy(r, b, 1 - c).wait_recv()
            return carry

        lax.fori_loop(0, 2, send, 0)
        lax.fori_loop(0, 2, receive, 0)
        lax.fori_loop(0, 2, finish, 0)

    def swapped(v):
        q = [v[j * quarter : (j + 1) * quarter] for j in range(4)]
        return jnp.concatenate([q[0], q[2], q[1], q[3]], axis=0)

    def mixer():
        edge = main + 128
        n = swapped(normed[...].reshape(rows, Dp))
        outer_inner = jnp.dot(n, g3[...], preferred_element_type=F32)
        outer_inner = outer_inner.astype(BF16).astype(F32)
        value_rest = jnp.dot(n, g4[:, 0:edge], preferred_element_type=F32)
        value_rest = value_rest.astype(BF16).astype(F32)
        rest = value_rest[:, main:]
        if rem:
            lane = lax.broadcasted_iota(jnp.int32, rest.shape, 1)
            keep = (lane >= 3 * rem) & (lane < 4 * rem)
            rests = [
                jnp.where(keep, pltpu.roll(rest, (3 - j) * rem, 1), 0.0) for j in range(3)
            ]
        else:
            rests = [jnp.zeros_like(rest)] * 3
        outer = jnp.concatenate([rests[0], outer_inner[:, 0:main]], axis=1)
        inner = jnp.concatenate([rests[1], outer_inner[:, main:]], axis=1)
        value = jnp.concatenate([rests[2], value_rest[:, 0:main]], axis=1)
        gated = inner * value
        token = lax.broadcasted_iota(jnp.int32, gated.shape, 0)
        conv = jnp.zeros_like(gated)
        for j in range(CONV_K):
            back = CONV_K - 1 - j
            moved = gated
            if back:
                moved = jnp.where(token >= back, pltpu.roll(gated, back, 0), 0.0)
            conv = conv + taps_ref[j : j + 1, :] * moved
        hidden[...] = swapped((outer * conv).astype(BF16)).reshape(hidden.shape)

    def mixer_block(b):
        acc[b] = lax.dot_general(hidden[b], g4[:, main:], NT, preferred_element_type=F32)

    def last_chunk(b):
        ffn_block(nff - 1, b, nff == 1)

    def second(b):
        acc[b] = jnp.zeros(acc.shape[1:], F32)

        def again(k, carry):
            ffn_block(k, b, False)
            return carry

        lax.fori_loop(0, nff, again, 0)

    for k in range(nff + 2):
        for owner, copy in local:
            if owner == k:
                copy.wait()
        if k < 2:
            own(k)
    norm_to(stream_ref, 0)
    for k in range(nff):
        zsteps(k)
        if k + 2 <= K3:
            own(k + 2)
        if k + 2 == K3:
            across(K4, z, go)
        if k > 0:
            wait_across(k - 1)
            ffn_chunk(k - 1, k == 1)
    zsteps(K3)
    start_a()
    steps_a(True)
    wait_across(nff - 1)
    reduce(0, last_chunk, stream_ref, 1, 0.5)
    norm_to(res.at[0], 2)
    wait_across(K3)
    steps_a(False)
    mixer()
    reduce(1, mixer_block, res.at[0], 3, 1.0)
    norm_to(res.at[1], 4)
    reduce(2, second, res.at[1], 5, 0.5)
    out_ref[...] = res[2]

    def done(copy):
        copy.wait_send()

    for k in range(nff + 1):
        def drain(s, carry):
            @pl.when(s <= z)
            def _():
                right(k, s, done)

            @pl.when(s >= z)
            def _():
                left(k, s, done)

            across(k, s, done)
            return carry

        lax.fori_loop(0, Z, drain, 0)
    across(K4, z, done)

    def drain_a(s, carry):
        @pl.when(s <= z)
        def _():
            right_a(s, done)

        @pl.when(s >= z)
        def _():
            left_a(s, done)

        return carry

    lax.fori_loop(0, Z, drain_a, 0)


def y_count(mesh):
    try:
        found = len({d.coords[1] for d in mesh.devices.reshape(-1)})
    except AttributeError:
        found = 1
    return found if found == 2 and mesh.shape["fs"] % 2 == 0 else 1


def solution(mesh):
    n_fs, n_tp = mesh.shape["fs"], mesh.shape["tp"]
    Y = y_count(mesh)
    Z, X = n_fs // Y, n_tp // 2

    def local(stream_in, norm_gains, gate, up, down, outer_w, inner_w, value_w, mixer_w, conv_taps):
        rows, width = stream_in.shape
        part, hid = gate.shape
        channels = outer_w.shape[1]
        shard = -(-part // 16) * 16
        Dp = n_fs * shard
        nff = 3 if hid % 384 == 0 else 1
        hc = hid // nff
        main = channels // 128 * 128
        rem = channels - main

        def widen(v):
            lead = v.shape[0]
            v = v.reshape(lead, n_fs, part)
            return jnp.pad(v, ((0, 0), (0, 0), (0, shard - part))).reshape(lead, Dp)

        sent = -(-part // 8) * 8

        def pack(w):
            return w if sent == part else jnp.pad(w, ((0, sent - part), (0, 0)))

        rest = [w[:, main:] for w in (outer_w, inner_w, value_w, mixer_w)]
        rest.append(jnp.zeros((part, 128 - 4 * rem), BF16))
        owns = [gate, up, down, outer_w, inner_w, value_w, mixer_w]
        owns = [pack(w) for w in owns + [jnp.concatenate(rest, axis=1)]]
        taps = lax.dynamic_slice_in_dim(
            conv_taps, lax.axis_index("tp") * channels, channels, 1
        ).astype(F32)
        taps = jnp.concatenate(
            [jnp.pad(taps[:, main:], ((0, 0), (3 * rem, 128 - 4 * rem))), taps[:, :main]], axis=1
        )
        half, quarter = rows // 2, rows // 4
        dma, vmem = pltpu.SemaphoreType.DMA, pltpu.VMEM
        out = pl.pallas_call(
            functools.partial(kernel, (Z, Y, X, shard, sent, width, hc, nff, main, rem)),
            out_shape=jax.ShapeDtypeStruct((rows, Dp), BF16),
            in_specs=[pl.BlockSpec(memory_space=pl.ANY)] * 8
            + [pl.BlockSpec(memory_space=pltpu.VMEM)] * 3,
            out_specs=pl.BlockSpec(memory_space=pltpu.VMEM),
            scratch_shapes=[
                vmem((nff, Dp, 3 * hc), BF16),
                vmem((Dp, 2 * main), BF16),
                vmem((Dp, 2 * main + 128), BF16),
                vmem((2, half, Dp), BF16),
                vmem((2, half, Dp), F32),
                vmem((2, half, main + 128), BF16),
                vmem((3, 2, quarter, Dp), BF16),
                vmem((3, 2, quarter, Dp), BF16),
                vmem((3, 2, quarter, Dp), BF16),
                vmem((3, 2, X - 1, quarter, Dp), BF16),
                vmem((3, rows, Dp), BF16),
                dma((3 * nff + 5,)),
                dma((nff + 2, 3, n_fs)),
                dma((nff + 2, n_fs)),
                dma((2, Z)),
                dma((Z,)),
                dma((2, 3, 2)),
                dma((3, 2, X - 1)),
                dma((3, 2, X - 1)),
                dma((2, 3, 2)),
            ],
            compiler_params=pltpu.CompilerParams(
                collective_id=0, has_side_effects=True, vmem_limit_bytes=60 * 1024 * 1024
            ),
        )(*owns, widen(stream_in), widen(norm_gains), taps)
        return out.reshape(rows, n_fs, shard)[:, :, :part].reshape(rows, width)

    return jax.shard_map(
        local,
        mesh=mesh,
        in_specs=(P("fs", None), P()) + (P("fs", "tp"),) * 7 + (P(),),
        out_specs=P("fs", None),
        check_vma=False,
    )
```

```python
import functools

import jax
import jax.numpy as jnp
from jax import lax
from jax.experimental import pallas as pl
from jax.experimental.pallas import tpu as pltpu
from jax.sharding import PartitionSpec as P

MESH = pl.DeviceIdType.MESH
EPSILON = 1e-06
CONV_K = 3
F32, BF16 = jnp.float32, jnp.bfloat16
NT = (((1,), (1,)), ((), ()))


def kernel(cfg, *refs):
    Z, Y, X, shard, sent, width, hc, nff, main, rem = cfg
    own_refs = refs[:8]
    stream_ref, gains_ref, taps_ref, out_ref = refs[8:12]
    (ff, g3, g4, normed, acc, hidden, csend, crecv, xsend, xrecv, res,
     lsem, zsend, recv, asend, arecv, csem, xssem, xrsem, rsem) = refs[12:]
    rows, Dp = stream_ref.shape
    half, quarter = rows // 2, rows // 4
    K3, K4 = nff, nff + 1
    f, t = lax.axis_index("fs"), lax.axis_index("tp")
    z, y = f // Y, f % Y
    c, x = t % 2, t // 2
    core_peer = (f, x * 2 + 1 - c)
    x_peers = [(f, ((x + j) % X) * 2 + c) for j in range(1, X)]

    def dev_z(zz):
        return (zz * Y + y, t)

    dev_y = (z * Y + (Y - 1 - y), t)

    for s in range(Z * Y):
        tail = pl.ds(s * shard + shard - 16, 16)
        for k in range(nff):
            ff[k, tail] = jnp.zeros((16, 3 * hc), BF16)
        g3[tail] = jnp.zeros((16, 2 * main), BF16)
        g4[tail] = jnp.zeros((16, 2 * main + 128), BF16)

    barrier = pltpu.get_barrier_semaphore()

    def greet(d):
        pl.semaphore_signal(barrier, inc=1, device_id=d, device_id_type=MESH)

    always = [core_peer] + x_peers + ([dev_y] if Y == 2 else [])
    for d in always:
        greet(d)
    if Z > 1:
        @pl.when(z > 0)
        def _():
            greet(dev_z(z - 1))

        @pl.when(z < Z - 1)
        def _():
            greet(dev_z(z + 1))

    def slot(k, first, count):
        at = pl.ds(pl.multiple_of(first * shard, 16), (count - 1) * shard + sent)
        if k < nff:
            return ff.at[k, at]
        return (g3 if k == K3 else g4).at[at]

    here = pl.ds(pl.multiple_of(f * shard, 16), sent)
    moves = []
    for k in range(nff):
        for j in range(3):
            moves.append((k, own_refs[j].at[:, pl.ds(k * hc, hc)],
                          ff.at[k, here, pl.ds(j * hc, hc)]))
    ow, iw, vw, mw, rw = own_refs[3:]
    lead = pl.ds(0, main)
    moves.append((K3, ow.at[:, lead], g3.at[here, lead]))
    moves.append((K3, iw.at[:, lead], g3.at[here, pl.ds(main, main)]))
    moves.append((K4, vw.at[:, lead], g4.at[here, lead]))
    moves.append((K4, rw, g4.at[here, pl.ds(main, 128)]))
    moves.append((K4, mw.at[:, lead], g4.at[here, pl.ds(main + 128, main)]))
    local = [
        (k, pltpu.make_async_copy(src, dst, lsem.at[n])) for n, (k, src, dst) in enumerate(moves)
    ]
    for _, copy in local:
        copy.start()

    peers = len(always)
    if Z > 1:
        peers = peers + (z > 0).astype(jnp.int32) + (z < Z - 1).astype(jnp.int32)
    pl.semaphore_wait(barrier, peers)

    def remote(k, s, way, d):
        ref = slot(k, s, 1)
        return pltpu.make_async_remote_copy(
            src_ref=ref, dst_ref=ref, send_sem=zsend.at[k, way, s], recv_sem=recv.at[k, s],
            device_id=d, device_id_type=MESH,
        )

    def remote_a(s, way, d):
        ref = slot(K4, s * Y, Y)
        return pltpu.make_async_remote_copy(
            src_ref=ref, dst_ref=ref, send_sem=asend.at[way, s], recv_sem=arecv.at[s],
            device_id=d, device_id_type=MESH,
        )

    def right(k, s, act):
        @pl.when(z < Z - 1)
        def _():
            act(remote(k, s * Y + y, 0, dev_z(z + 1)))

    def left(k, s, act):
        @pl.when(z > 0)
        def _():
            act(remote(k, s * Y + y, 1, dev_z(z - 1)))

    def across(k, s, act):
        if Y == 2:
            act(remote(k, s * Y + y, 2, dev_y))

    def go(copy):
        copy.start()

    def own(k):
        right(k, z, go)
        left(k, z, go)
        across(k, z, go)

    def zsteps(k):
        def step(i, carry):
            @pl.when(z - 1 - i >= 0)
            def _():
                s = z - 1 - i
                remote(k, s * Y + y, 0, dev_z(z - 1)).wait_recv()
                right(k, s, go)
                across(k, s, go)

            @pl.when(z + 1 + i < Z)
            def _():
                s = z + 1 + i
                remote(k, s * Y + y, 0, dev_z(z + 1)).wait_recv()
                left(k, s, go)
                across(k, s, go)

            return carry

        lax.fori_loop(0, Z - 1, step, 0)

    def wait_across(k):
        if Y == 2:
            def step(s, carry):
                remote(k, s * Y + 1 - y, 2, dev_y).wait_recv()
                return carry

            lax.fori_loop(0, Z, step, 0)

    def right_a(s, act):
        @pl.when(z < Z - 1)
        def _():
            act(remote_a(s, 0, dev_z(z + 1)))

    def left_a(s, act):
        @pl.when(z > 0)
        def _():
            act(remote_a(s, 1, dev_z(z - 1)))

    def start_a():
        if Y == 2:
            remote(K4, z * Y + 1 - y, 2, dev_y).wait_recv()
        right_a(z, go)
        left_a(z, go)

    def steps_a(forward):
        def step(i, carry):
            @pl.when((z - 1 - i >= 0) & ((z < Z - 1) if forward else (z == Z - 1)))
            def _():
                s = z - 1 - i
                remote_a(s, 0, dev_z(z - 1)).wait_recv()
                if forward:
                    right_a(s, go)

            @pl.when((z + 1 + i < Z) & ((z > 0) if forward else (z == 0)))
            def _():
                s = z + 1 + i
                remote_a(s, 0, dev_z(z + 1)).wait_recv()
                if forward:
                    left_a(s, go)

            return carry

        lax.fori_loop(0, Z - 1, step, 0)

    def scaled(values, row):
        mean = jnp.sum(values * values, axis=-1, keepdims=True) * (1.0 / width)
        return values * lax.rsqrt(mean + EPSILON) * gains_ref[row : row + 1, :]

    def norm_to(source, row):
        def block(i, carry):
            at = pl.ds(pl.multiple_of(i * 32, 32), 32)
            per_half, per_quarter = half // 32, quarter // 32
            h, b = i // per_half, (i % per_half) // per_quarter
            to = pl.ds(pl.multiple_of(h * quarter + (i % per_quarter) * 32, 32), 32)
            normed[b, to] = scaled(source[at].astype(F32), row).astype(BF16)
            return carry

        lax.fori_loop(0, rows // 32, block, 0)

    def ffn_block(k, b, first):
        weights = ff.at[k]
        n = normed[b]
        gate = jnp.dot(n, weights[:, 0:hc], preferred_element_type=F32)
        up = jnp.dot(n, weights[:, hc : 2 * hc], preferred_element_type=F32)
        h = (gate / (1.0 + jnp.exp(-gate)) * up).astype(BF16)
        part = lax.dot_general(h, weights[:, 2 * hc :], NT, preferred_element_type=F32)
        acc[b] = part if first else acc[b] + part

    def ffn_chunk(k, first):
        def block(b, carry):
            ffn_block(k, b, first)
            return carry

        lax.fori_loop(0, 2, block, 0)

    mine = pl.ds(pl.multiple_of(c * quarter, 16), quarter)
    other = pl.ds(pl.multiple_of((1 - c) * quarter, 16), quarter)

    def core_copy(r, b):
        return pltpu.make_async_remote_copy(
            src_ref=csend.at[r, b], dst_ref=crecv.at[r, b], send_sem=csem.at[0, r, b],
            recv_sem=csem.at[1, r, b], device_id=core_peer, device_id_type=MESH,
        )

    def x_copy(r, b, j):
        return pltpu.make_async_remote_copy(
            src_ref=xsend.at[r, b], dst_ref=xrecv.at[r, b, j], send_sem=xssem.at[r, b, j],
            recv_sem=xrsem.at[r, b, j], device_id=x_peers[j], device_id_type=MESH,
        )

    def res_copy(r, b, core):
        at = pl.ds(pl.multiple_of(core * half + b * quarter, 16), quarter)
        return pltpu.make_async_remote_copy(
            src_ref=res.at[r, at], dst_ref=res.at[r, at], send_sem=rsem.at[0, r, b],
            recv_sem=rsem.at[1, r, b], device_id=core_peer, device_id_type=MESH,
        )

    def reduce(r, compute, source, row, factor):
        def send(b, carry):
            compute(b)
            csend[r, b] = acc[b, other].astype(BF16)
            core_copy(r, b).start()
            core_copy(r, b).wait()
            xsend[r, b] = (
                acc[b, mine].astype(BF16).astype(F32) + crecv[r, b].astype(F32)
            ).astype(BF16)
            for j in range(X - 1):
                x_copy(r, b, j).start()
            return carry

        def receive(b, carry):
            for j in range(X - 1):
                x_copy(r, b, j).wait()

            def block(i, inner_carry):
                at = pl.ds(pl.multiple_of(i * 32, 16), 32)
                full = pl.ds(pl.multiple_of(c * half + b * quarter + i * 32, 16), 32)
                total = xsend[r, b, at].astype(F32)
                for j in range(X - 1):
                    total = total + xrecv[r, b, j, at].astype(F32)
                res[r, full] = (
                    source[full].astype(F32) + factor * scaled(total, row)
                ).astype(BF16)
                return inner_carry

            lax.fori_loop(0, quarter // 32, block, 0)
            res_copy(r, b, c).start()
            return carry

        def finish(b, carry):
            res_copy(r, b, c).wait_send()
            res_copy(r, b, 1 - c).wait_recv()
            return carry

        lax.fori_loop(0, 2, send, 0)
        lax.fori_loop(0, 2, receive, 0)
        lax.fori_loop(0, 2, finish, 0)

    def swapped(v):
        q = [v[j * quarter : (j + 1) * quarter] for j in range(4)]
        return jnp.concatenate([q[0], q[2], q[1], q[3]], axis=0)

    def mixer():
        wait_across(K3)
        edge = main + 128
        n = swapped(normed[...].reshape(rows, Dp))
        outer_inner = jnp.dot(n, g3[...], preferred_element_type=F32)
        outer_inner = outer_inner.astype(BF16).astype(F32)
        steps_a(False)
        value_rest = jnp.dot(n, g4[:, 0:edge], preferred_element_type=F32)
        value_rest = value_rest.astype(BF16).astype(F32)
        rest = value_rest[:, main:]
        if rem:
            lane = lax.broadcasted_iota(jnp.int32, rest.shape, 1)
            keep = (lane >= 3 * rem) & (lane < 4 * rem)
            rests = [
                jnp.where(keep, pltpu.roll(rest, (3 - j) * rem, 1), 0.0) for j in range(3)
            ]
        else:
            rests = [jnp.zeros_like(rest)] * 3
        outer = jnp.concatenate([rests[0], outer_inner[:, 0:main]], axis=1)
        inner = jnp.concatenate([rests[1], outer_inner[:, main:]], axis=1)
        value = jnp.concatenate([rests[2], value_rest[:, 0:main]], axis=1)
        gated = inner * value
        token = lax.broadcasted_iota(jnp.int32, gated.shape, 0)
        conv = jnp.zeros_like(gated)
        for j in range(CONV_K):
            back = CONV_K - 1 - j
            moved = gated
            if back:
                moved = jnp.where(token >= back, pltpu.roll(gated, back, 0), 0.0)
            conv = conv + taps_ref[j : j + 1, :] * moved
        hidden[...] = swapped((outer * conv).astype(BF16)).reshape(hidden.shape)

    def mixer_block(b):
        acc[b] = lax.dot_general(hidden[b], g4[:, main:], NT, preferred_element_type=F32)

    def last_chunk(b):
        ffn_block(nff - 1, b, nff == 1)

    def second(b):
        acc[b] = jnp.zeros(acc.shape[1:], F32)

        def again(k, carry):
            ffn_block(k, b, False)
            return carry

        lax.fori_loop(0, nff, again, 0)

    for k in range(nff + 2):
        for owner, copy in local:
            if owner == k:
                copy.wait()
        if k < 2:
            own(k)
    norm_to(stream_ref, 0)
    for k in range(nff):
        zsteps(k)
        if k + 2 <= K3:
            own(k + 2)
        if k == 0:
            across(K4, z, go)
        if k == 1 and nff > 2:
            wait_across(0)
            ffn_chunk(0, True)
    start_a()
    zsteps(K3)
    steps_a(True)
    for k in range(1 if nff > 2 else 0, nff - 1):
        wait_across(k)
        ffn_chunk(k, k == 0)
    wait_across(nff - 1)
    reduce(0, last_chunk, stream_ref, 1, 0.5)
    norm_to(res.at[0], 2)
    mixer()
    reduce(1, mixer_block, res.at[0], 3, 1.0)
    norm_to(res.at[1], 4)
    reduce(2, second, res.at[1], 5, 0.5)
    out_ref[...] = res[2]

    def done(copy):
        copy.wait_send()

    for k in range(nff + 1):
        def drain(s, carry):
            @pl.when(s <= z)
            def _():
                right(k, s, done)

            @pl.when(s >= z)
            def _():
                left(k, s, done)

            across(k, s, done)
            return carry

        lax.fori_loop(0, Z, drain, 0)
    across(K4, z, done)

    def drain_a(s, carry):
        @pl.when(s <= z)
        def _():
            right_a(s, done)

        @pl.when(s >= z)
        def _():
            left_a(s, done)

        return carry

    lax.fori_loop(0, Z, drain_a, 0)


def y_count(mesh):
    try:
        found = len({d.coords[1] for d in mesh.devices.reshape(-1)})
    except AttributeError:
        found = 1
    return found if found == 2 and mesh.shape["fs"] % 2 == 0 else 1


def solution(mesh):
    n_fs, n_tp = mesh.shape["fs"], mesh.shape["tp"]
    Y = y_count(mesh)
    Z, X = n_fs // Y, n_tp // 2

    def local(stream_in, norm_gains, gate, up, down, outer_w, inner_w, value_w, mixer_w, conv_taps):
        rows, width = stream_in.shape
        part, hid = gate.shape
        channels = outer_w.shape[1]
        shard = -(-part // 16) * 16
        Dp = n_fs * shard
        nff = 3 if hid % 384 == 0 else 1
        hc = hid // nff
        main = channels // 128 * 128
        rem = channels - main

        def widen(v):
            lead = v.shape[0]
            v = v.reshape(lead, n_fs, part)
            return jnp.pad(v, ((0, 0), (0, 0), (0, shard - part))).reshape(lead, Dp)

        sent = -(-part // 8) * 8

        def pack(w):
            return w if sent == part else jnp.pad(w, ((0, sent - part), (0, 0)))

        rest = [w[:, main:] for w in (outer_w, inner_w, value_w, mixer_w)]
        rest.append(jnp.zeros((part, 128 - 4 * rem), BF16))
        owns = [gate, up, down, outer_w, inner_w, value_w, mixer_w]
        owns = [pack(w) for w in owns + [jnp.concatenate(rest, axis=1)]]
        taps = lax.dynamic_slice_in_dim(
            conv_taps, lax.axis_index("tp") * channels, channels, 1
        ).astype(F32)
        taps = jnp.concatenate(
            [jnp.pad(taps[:, main:], ((0, 0), (3 * rem, 128 - 4 * rem))), taps[:, :main]], axis=1
        )
        half, quarter = rows // 2, rows // 4
        dma, vmem = pltpu.SemaphoreType.DMA, pltpu.VMEM
        out = pl.pallas_call(
            functools.partial(kernel, (Z, Y, X, shard, sent, width, hc, nff, main, rem)),
            out_shape=jax.ShapeDtypeStruct((rows, Dp), BF16),
            in_specs=[pl.BlockSpec(memory_space=pl.ANY)] * 8
            + [pl.BlockSpec(memory_space=pltpu.VMEM)] * 3,
            out_specs=pl.BlockSpec(memory_space=pltpu.VMEM),
            scratch_shapes=[
                vmem((nff, Dp, 3 * hc), BF16),
                vmem((Dp, 2 * main), BF16),
                vmem((Dp, 2 * main + 128), BF16),
                vmem((2, half, Dp), BF16),
                vmem((2, half, Dp), F32),
                vmem((2, half, main + 128), BF16),
                vmem((3, 2, quarter, Dp), BF16),
                vmem((3, 2, quarter, Dp), BF16),
                vmem((3, 2, quarter, Dp), BF16),
                vmem((3, 2, X - 1, quarter, Dp), BF16),
                vmem((3, rows, Dp), BF16),
                dma((3 * nff + 5,)),
                dma((nff + 2, 3, n_fs)),
                dma((nff + 2, n_fs)),
                dma((2, Z)),
                dma((Z,)),
                dma((2, 3, 2)),
                dma((3, 2, X - 1)),
                dma((3, 2, X - 1)),
                dma((2, 3, 2)),
            ],
            compiler_params=pltpu.CompilerParams(
                collective_id=0, has_side_effects=True, vmem_limit_bytes=60 * 1024 * 1024
            ),
        )(*owns, widen(stream_in), widen(norm_gains), taps)
        return out.reshape(rows, n_fs, shard)[:, :, :part].reshape(rows, width)

    return jax.shard_map(
        local,
        mesh=mesh,
        in_specs=(P("fs", None), P()) + (P("fs", "tp"),) * 7 + (P(),),
        out_specs=P("fs", None),
        check_vma=False,
    )
```
